32 devices in a mesh: gr: 2 (over core), fs: 8 (over z, y), tp: 2 (over x).
Axes of the slice: x: 2, y: 2, z: 4, core: 2. Of those that a mesh axis runs over, the one named last changes fastest.
Arguments:
- tokens: bfloat16 [2048, 2048], P(('gr', 'fs')), may hold values from -6 to 6
- norm_gain: float32 [2048], P(('gr', 'fs')), may hold values from 0.1 to 1.9
- gate_train: float32 [32, 2048, 1024], P(None, ('gr', 'fs'), 'tp'), may hold values from -0.3125 to 0.3125
- up_train: float32 [32, 2048, 1024], P(None, ('gr', 'fs'), 'tp'), may hold values from -0.3125 to 0.3125
- down_train: float32 [32, 1024, 2048], P(None, ('gr', 'fs'), 'tp'), may hold values from -0.09375 to 0.09375
- routes: int32 [2048, 4], P(('gr', 'fs')), may hold values from 0 to 31, all different within a row; in each aligned block of 128 rows (0 to 127, 128 to 255, ...) at most 32 rows name the same one
- route_weight: float32 [2048, 4], P(('gr', 'fs')), may hold values from 0.05 to 1
Outputs:
- mixed: bfloat16 [2048, 2048], P(('gr', 'fs'), 'tp')
- gate_packed: bfloat16 [32, 2048, 1024], P('fs', None, 'tp')
- up_packed: bfloat16 [32, 2048, 1024], P('fs', None, 'tp')
- down_packed: bfloat16 [32, 1024, 2048], P('fs', 'tp')
The draws below stay inside these ranges and needn't reach their ends.
Inputs may be any that keep to these rules, and one draw needn't show every extreme that they name: `routes`: each row names 4 different experts. Among the rows of one device no expert is named more than 32 times, and in every draw some expert is named exactly 32 times by the rows of some device.
All inputs are finite; a program needn't handle non-finite values.
Results may differ from the reference program's by a relative error of at most 0.015.
Values may be sent and summed in bfloat16 or wider, within the bound.
A program may use at most 128 MiB of HBM per device.

```python
import math
import jax
import jax.numpy as jnp
import numpy as np
from jax import lax

D = 2048
FF = 1024
EXPERTS = 32
TOP = 4
TOK_DEV = 128
CAP = 32
TOKENS = 2048
N_TP = 2


def levels(rng, dims, shards, least, top_value):
    def one(position, blocks):
        draws = jax.random.uniform(jax.random.fold_in(jax.random.fold_in(rng, 6), position), (blocks,), jnp.float32, least / len(shards), top_value / len(shards))
        return jnp.repeat(jnp.exp(draws), dims[position] // blocks).reshape((-1,) + (1,) * (len(dims) - position - 1))

    level = one(*shards[0])
    for cut in shards[1:]:
        level = level * one(*cut)
    return level


def assign_block(stream_key, own, number, rows, number_of, top, most, slope):
    sequence = jax.random.permutation(stream_key, number_of)
    heavy_load, usual = load_shares(number_of, rows * top, most, slope, True), load_shares(number_of, rows * top, most, slope, False)
    places = jnp.arange(number_of)

    def named(sizes, rotation):
        used = int((sizes > 0).sum())
        fixed = max(1, used // 4)
        moved = fixed + (places - fixed + rotation * (used - fixed)) % max(1, number_of - fixed)
        return jnp.zeros((number_of,), jnp.int32).at[sequence[jnp.where(places < fixed, places, moved)]].set(jnp.asarray(sizes, jnp.int32))

    sizes = jnp.where(number % 4 == 0, named(heavy_load, number // 4), named(usual, number - number // 4 - 1))
    mixed = jax.random.permutation(jax.random.fold_in(own, 3), number_of)
    source_of, receiver = mixed[0:number_of // 2 * 2:2], mixed[1:number_of // 2 * 2:2]
    room = jnp.minimum(sizes[source_of] - 1, most - sizes[receiver]) // 2
    room = jnp.where((source_of == sequence[0]) | (receiver == sequence[0]) | (sizes[receiver] == 0), 0, jnp.maximum(room, 0))
    moved = jax.random.randint(jax.random.fold_in(own, 4), (number_of // 2,), 0, 1 << 20) % (room + 1)
    sizes = sizes.at[source_of].add(-moved).at[receiver].add(moved)
    members = jnp.searchsorted(jnp.cumsum(sizes), jnp.arange(rows * top), side="right").astype(jnp.int32)
    listing = members.reshape(top, rows).T
    listing = listing[jax.random.permutation(jax.random.fold_in(own, 1), rows)]
    rotation = jax.random.randint(jax.random.fold_in(own, 2), (rows, 1), 0, top)
    return jnp.take_along_axis(listing, (jnp.arange(top)[None, :] + rotation) % top, axis=1)


def load_shares(amount, total, bound, slope, full):
    portions = [(1 << 20) // math.isqrt(standing ** slope) + 1 for standing in range(1, amount + 1)]
    largest = bound if full else min(bound, max(-(-total // amount), total * portions[0] // sum(portions)))
    least = 1 if total - largest >= amount - 1 else 0
    holding, rest = [largest] + [least] * (amount - 1), total - largest - least * (amount - 1)
    while rest > 0:
        movable = [i for i in range(1, amount) if holding[i] < largest] or [i for i in range(1, amount) if holding[i] < bound]
        mass, left = sum([portions[i] for i in movable]), rest
        for i in movable:
            extra = min(bound - holding[i], max(1, left * portions[i] // mass), rest)
            holding[i] = holding[i] + extra
            rest = rest - extra
    return np.array(holding)


def gaussian(rng, shape, width, bound, pieces=(), held_as=jnp.bfloat16):
    entries = width * jax.random.normal(rng, shape, jnp.float32)
    if pieces:
        entries = entries * levels(rng, shape, pieces, -0.22, 0.18)
    return jnp.clip(entries, -bound, bound).astype(held_as)


def setup_inputs(seed: int = 0) -> dict:
    splits = jax.random.split(jax.random.key(seed), 8)
    tokens = gaussian(splits[0], (TOKENS, D), 1.0, 6.0, ((0, 16),))
    norm_gain = jnp.clip(1.0 + 0.18 * jax.random.normal(splits[1], (D,), jnp.float32), 0.1, 1.9)
    gate_train = gaussian(splits[2], (EXPERTS, D, FF), (D // 6) ** -0.5, 0.3125, ((1, 16), (2, 2)), jnp.float32)
    up_train = gaussian(splits[3], (EXPERTS, D, FF), (D // 6) ** -0.5, 0.3125, ((1, 16), (2, 2)), jnp.float32)
    down_train = gaussian(splits[4], (EXPERTS, FF, D), (FF * 4) ** -0.5, 0.09375, ((1, 16), (2, 2)), jnp.float32)
    routes_keys = jax.random.split(jax.random.fold_in(splits[5], 1), TOKENS // TOK_DEV)
    routes_turns = jax.random.permutation(jax.random.fold_in(splits[5], 3), TOKENS // TOK_DEV)
    routes = jax.vmap(lambda own, number: assign_block(jax.random.fold_in(splits[5], 2), own, number, TOK_DEV, EXPERTS, TOP, CAP, 2))(routes_keys, routes_turns).reshape((TOKENS, TOP))
    route_weight = jnp.clip(jnp.exp(math.log(1.0) - 2.9957323 * jax.random.uniform(splits[6], (TOKENS, TOP), jnp.float32) ** levels(splits[6], (TOKENS, TOP), ((0, 16),), -0.2, 0.2)), 0.05, 1.0)
    return dict(tokens=tokens, norm_gain=norm_gain, gate_train=gate_train, up_train=up_train, down_train=down_train, routes=routes, route_weight=route_weight)


CLAMP_LIMIT = 7.0
SLOPE_ALPHA = 1.702
NORM_EPSILON = 1e-06

def reference(tokens, norm_gain, gate_train, up_train, down_train, routes, route_weight):
    gate_packed = (norm_gain[None, :, None] * gate_train).astype(jnp.bfloat16)
    up_packed = (norm_gain[None, :, None] * up_train).astype(jnp.bfloat16)
    down_packed = down_train.astype(jnp.bfloat16)
    tokens_wide = tokens.astype(jnp.float32)
    normed = (tokens_wide * lax.rsqrt(lax.optimization_barrier(jnp.mean(tokens_wide * tokens_wide, axis=1, keepdims=True)) + NORM_EPSILON)).astype(jnp.bfloat16)
    blocks = TOKENS // TOK_DEV
    flat_routes = routes.reshape(blocks, TOK_DEV * TOP)
    one_hot = (flat_routes[:, :, None] == jnp.arange(EXPERTS, dtype=jnp.int32)[None, None, :]).astype(jnp.int32)
    counts = jnp.cumsum(one_hot, axis=1)
    slot_index = lax.optimization_barrier(jnp.sum((counts - 1) * one_hot, axis=2))
    expert_rows = blocks * CAP
    target_rows = (flat_routes * expert_rows + jnp.arange(blocks, dtype=jnp.int32)[:, None] * CAP + slot_index).reshape(-1).astype(jnp.int32)
    copied_rows = jnp.repeat(normed, TOP, axis=0)
    dispatch_buffer = jnp.zeros((EXPERTS * expert_rows, D), jnp.bfloat16).at[target_rows].set(copied_rows)
    dispatch_buffer = dispatch_buffer.reshape(EXPERTS, expert_rows, D)
    block_width = FF // N_TP

    def expert(operands):
        inputs, gate_weight, up_weight, down_weight = operands
        gate_pre = jnp.dot(inputs, gate_weight, preferred_element_type=jnp.float32)
        up_pre = jnp.dot(inputs, up_weight, preferred_element_type=jnp.float32)
        clipped = jnp.minimum(gate_pre, CLAMP_LIMIT)
        hidden = ((jnp.clip(up_pre, -CLAMP_LIMIT, CLAMP_LIMIT) + 1.0) * clipped * jax.nn.sigmoid(SLOPE_ALPHA * clipped)).astype(jnp.bfloat16)
        summed = jnp.zeros((inputs.shape[0], D), jnp.float32)
        for block in range(N_TP):
            partial_value = jnp.dot(hidden[:, block * block_width:(block + 1) * block_width], down_weight[block * block_width:(block + 1) * block_width], preferred_element_type=jnp.float32).astype(jnp.bfloat16)
            partial_value = lax.optimization_barrier(partial_value)
            summed = summed + partial_value.astype(jnp.float32)
        return summed.astype(jnp.bfloat16)
    results = lax.map(expert, (dispatch_buffer, gate_packed, up_packed, down_packed))
    picked = results.reshape(EXPERTS * expert_rows, D)[target_rows].reshape(TOKENS, TOP, D).astype(jnp.float32)
    mixed = lax.optimization_barrier(jnp.sum(picked * route_weight[:, :, None], axis=1)).astype(jnp.bfloat16)
    return (mixed, gate_packed, up_packed, down_packed)
```

```python
import jax
import jax.numpy as jnp
from jax import lax
from jax.sharding import PartitionSpec as P

CAP = 32
CLAMP_LIMIT = 7.0
SLOPE_ALPHA = 1.702
NORM_EPSILON = 1e-06


def solution(mesh):
    gr_n, fs_n, tp_n = mesh.shape["gr"], mesh.shape["fs"], mesh.shape["tp"]

    def body(tokens, norm_gain, gate_train, up_train, down_train, routes, route_weight):
        experts = gate_train.shape[0]
        local_experts = experts // fs_n
        rows, width = tokens.shape
        gate_local = (norm_gain[None, :, None] * gate_train).astype(jnp.bfloat16)
        gate_part = lax.all_to_all(gate_local, "fs", split_axis=0, concat_axis=1, tiled=True)

        tokens_wide = tokens.astype(jnp.float32)
        normed = (
            tokens_wide
            * lax.rsqrt(jnp.mean(tokens_wide * tokens_wide, axis=1, keepdims=True) + NORM_EPSILON)
        ).astype(jnp.bfloat16)
        normed_all = lax.all_gather(normed, "fs", axis=0, tiled=False)
        routing = jnp.concatenate([routes.astype(jnp.float32), route_weight], axis=1)
        routing_all = lax.all_gather(routing, "fs", axis=0, tiled=False)
        top = routes.shape[1]
        routes_all = routing_all[:, :, :top].astype(jnp.int32)
        weight_all = routing_all[:, :, top:]
        mine = lax.axis_index("fs") * local_experts + jnp.arange(local_experts, dtype=jnp.int32)
        hit = routes_all[:, :, :, None] == mine[None, None, None, :]
        chosen = jnp.any(hit, axis=2)
        share = jnp.sum(jnp.where(hit, weight_all[:, :, :, None], 0.0), axis=2)
        lower = (jnp.arange(rows)[:, None] >= jnp.arange(rows)[None, :]).astype(jnp.bfloat16)
        count = jnp.einsum(
            "st,btj->bsj", lower, chosen.astype(jnp.bfloat16), preferred_element_type=jnp.float32
        )
        slot = jnp.where(chosen, count.astype(jnp.int32) - 1, -1)
        place = slot[:, :, :, None] == jnp.arange(CAP, dtype=jnp.int32)[None, None, None, :]
        pick = place.astype(jnp.bfloat16)
        spread = jnp.where(place, share[:, :, :, None], 0.0).astype(jnp.bfloat16)
        arrived = jnp.einsum(
            "btjc,btd->bjcd", pick, normed_all, preferred_element_type=jnp.float32
        ).astype(jnp.bfloat16)
        arrived = arrived.transpose(1, 0, 2, 3).reshape(local_experts, fs_n * CAP, width)

        gate_part, norm_gain, up_train = lax.optimization_barrier((gate_part, norm_gain, up_train))
        up_local = (norm_gain[None, :, None] * up_train).astype(jnp.bfloat16)
        up_part = lax.all_to_all(up_local, "fs", split_axis=0, concat_axis=1, tiled=True)
        gate_weight = lax.all_gather(gate_part, "gr", axis=1, tiled=True)
        up_part, down_train = lax.optimization_barrier((up_part, down_train))
        down_local = down_train.astype(jnp.bfloat16)
        down_part = lax.all_to_all(down_local, "fs", split_axis=0, concat_axis=1, tiled=True)
        up_weight = lax.all_gather(up_part, "gr", axis=1, tiled=True)

        gate_pre = jnp.einsum(
            "erd,edf->erf", arrived, gate_weight, preferred_element_type=jnp.float32
        )
        up_pre = jnp.einsum("erd,edf->erf", arrived, up_weight, preferred_element_type=jnp.float32)
        clipped = jnp.minimum(gate_pre, CLAMP_LIMIT)
        hidden = (
            (jnp.clip(up_pre, -CLAMP_LIMIT, CLAMP_LIMIT) + 1.0)
            * clipped
            * jax.nn.sigmoid(SLOPE_ALPHA * clipped)
        ).astype(jnp.bfloat16)
        hidden_all = lax.all_gather(hidden, "tp", axis=2, tiled=True)

        down_cols = lax.all_gather(down_part, "gr", axis=1, tiled=True)
        if gr_n == tp_n:
            swap = [(g * tp_n + t, t * tp_n + g) for g in range(gr_n) for t in range(tp_n)]
            turned = lax.ppermute(down_part, ("gr", "tp"), swap)
            down_weight = lax.all_gather(turned, "gr", axis=2, tiled=True)
        else:
            down_weight = lax.all_to_all(
                down_cols, "tp", split_axis=1, concat_axis=2, tiled=True
            )

        results = jnp.einsum(
            "erf,efd->erd", hidden_all, down_cols, preferred_element_type=jnp.float32
        ).astype(jnp.bfloat16)
        features = results.shape[2]
        results = results.reshape(local_experts, fs_n, CAP, features)
        partial_mix = jnp.einsum(
            "btjc,jbcd->btd", spread, results, preferred_element_type=jnp.float32
        ).astype(jnp.bfloat16)
        mixed = lax.psum_scatter(
            partial_mix.reshape(fs_n * rows, features), "fs", scatter_dimension=0, tiled=True
        )
        return (mixed, gate_weight, up_weight, down_weight)

    placed = (
        P(("gr", "fs"), None),
        P(("gr", "fs")),
        P(None, ("gr", "fs"), "tp"),
        P(None, ("gr", "fs"), "tp"),
        P(None, ("gr", "fs"), "tp"),
        P(("gr", "fs"), None),
        P(("gr", "fs"), None),
    )
    return jax.shard_map(
        body,
        mesh=mesh,
        in_specs=placed,
        out_specs=(
            P(("gr", "fs"), "tp"),
            P("fs", None, "tp"),
            P("fs", None, "tp"),
            P("fs", "tp", None),
        ),
        check_vma=False,
    )
```

```python
import jax
import jax.numpy as jnp
from jax import lax
from jax.experimental import pallas as pl
from jax.experimental.pallas import tpu as pltpu
from jax.sharding import PartitionSpec as P

EXPERTS = 32
TOP = 4
CAP = 32
CLAMP_LIMIT = 7.0
SLOPE_ALPHA = 1.702
NORM_EPSILON = 1e-06
MESH = pl.DeviceIdType.MESH
STEPS = (2, 3, 1, 6, 7, 4, 5)


def plain_body(tokens, norm_gain, gate_train, up_train, down_train, routes, route_weight):
    gate_local = (norm_gain[None, :, None] * gate_train).astype(jnp.bfloat16)
    up_local = (norm_gain[None, :, None] * up_train).astype(jnp.bfloat16)
    down_local = down_train.astype(jnp.bfloat16)
    served = (
        lax.all_to_all(gate_local, "fs", split_axis=0, concat_axis=1, tiled=True),
        lax.all_to_all(up_local, "fs", split_axis=0, concat_axis=1, tiled=True),
        lax.all_to_all(down_local, "fs", split_axis=0, concat_axis=1, tiled=True),
    )
    gate_weight, up_weight, down_cols = (
        lax.all_gather(served[0], "gr", axis=1, tiled=True),
        lax.all_gather(served[1], "gr", axis=1, tiled=True),
        lax.all_gather(served[2], "gr", axis=1, tiled=True),
    )
    down_weight = lax.all_to_all(down_cols, "tp", split_axis=1, concat_axis=2, tiled=True)
    tokens_wide = tokens.astype(jnp.float32)
    normed = (
        tokens_wide
        * lax.rsqrt(jnp.mean(tokens_wide * tokens_wide, axis=1, keepdims=True) + NORM_EPSILON)
    ).astype(jnp.bfloat16)
    flat_routes = routes.reshape(-1)
    one_hot = (flat_routes[:, None] == jnp.arange(EXPERTS, dtype=jnp.int32)[None, :]).astype(
        jnp.int32
    )
    counts = jnp.cumsum(one_hot, axis=0)
    slot_index = jnp.sum((counts - 1) * one_hot, axis=1)
    target_rows = flat_routes * CAP + slot_index
    copied_rows = jnp.repeat(normed, TOP, axis=0)
    dispatch_buffer = (
        jnp.zeros((EXPERTS * CAP, normed.shape[1]), jnp.bfloat16).at[target_rows].set(copied_rows)
    )
    dispatch_buffer = dispatch_buffer.reshape(EXPERTS, CAP, normed.shape[1])
    arrived = lax.all_to_all(dispatch_buffer, "fs", split_axis=0, concat_axis=1, tiled=True)
    gate_pre = jnp.einsum("erd,edf->erf", arrived, gate_weight, preferred_element_type=jnp.float32)
    up_pre = jnp.einsum("erd,edf->erf", arrived, up_weight, preferred_element_type=jnp.float32)
    clipped = jnp.minimum(gate_pre, CLAMP_LIMIT)
    hidden = (
        (jnp.clip(up_pre, -CLAMP_LIMIT, CLAMP_LIMIT) + 1.0)
        * clipped
        * jax.nn.sigmoid(SLOPE_ALPHA * clipped)
    ).astype(jnp.bfloat16)
    partial_value = jnp.einsum(
        "erf,efd->erd", hidden, down_weight, preferred_element_type=jnp.float32
    )
    summed = lax.psum_scatter(
        partial_value.astype(jnp.bfloat16), "tp", scatter_dimension=2, tiled=True
    )
    returned = lax.all_to_all(summed, "fs", split_axis=1, concat_axis=0, tiled=True)
    features = returned.shape[2]
    picked = (
        returned.reshape(EXPERTS * CAP, features)[target_rows]
        .reshape(tokens.shape[0], TOP, features)
        .astype(jnp.float32)
    )
    mixed = jnp.sum(picked * route_weight[:, :, None], axis=1).astype(jnp.bfloat16)
    return (mixed, gate_weight, up_weight, down_weight)


def flip(fs, step):
    z, y = lax.div(fs, 2), lax.rem(fs, 2)
    if step % 2:
        y = 1 - y
    if step // 2 == 3:
        z = 3 - z
    elif step // 2 == 2:
        z = lax.rem(z + 2, 4)
    elif step // 2 == 1:
        z = z + 1 - 2 * lax.rem(z, 2)
    return z * 2 + y


def exchange_kernel(
    normed, routing, gate, up, down,
    normed_all, routing_all, gate_out, up_out, down_out,
    send, recv, relay_send, relay_recv, local_sem, tok_send, tok_recv, route_send, route_recv,
):
    g, f, t = lax.axis_index("gr"), lax.axis_index("fs"), lax.axis_index("tp")
    local_experts = gate_out.shape[0]
    fs_n = 8
    rows, down_rows = gate.shape[1], down.shape[1]
    wide = down.shape[2]
    half = normed.shape[1] // 2

    barrier = pltpu.get_barrier_semaphore()

    def greet(device):
        pl.semaphore_signal(barrier, inc=1, device_id=device, device_id_type=MESH)

    for step in STEPS:
        greet((g, flip(f, step), t))
    for step in range(fs_n):
        greet((1 - g, flip(f, step), 1 - t))
    greet((1 - g, f, t))
    greet((g, f, 1 - t))
    pl.semaphore_wait(barrier, 17)

    def remote(src, dst, s, r, device):
        return pltpu.make_async_remote_copy(
            src_ref=src, dst_ref=dst, send_sem=s, recv_sem=r, device_id=device, device_id_type=MESH
        )

    def tok(block):
        return normed_all.at[block, :, pl.ds(pl.multiple_of(t * half, half), half)]

    own_half = normed.at[:, pl.ds(pl.multiple_of(t * half, half), half)]
    first = {s: remote(own_half, tok(f), tok_send.at[s], tok_recv.at[s], (g, flip(f, s), t))
             for s in (2, 4, 6)}
    for s in (6, 4, 2):
        first[s].start()
    small = {s: remote(routing, routing_all.at[f], route_send.at[s], route_recv.at[s],
                       (g, flip(f, s), t)) for s in STEPS}
    for s in STEPS:
        small[s].start()

    def gate_at(whole, group, owner):
        return whole.at[:, pl.ds(pl.multiple_of((group * fs_n + owner) * rows, rows), rows), :]

    def down_at(owner, group):
        return down_out.at[
            :,
            pl.ds(pl.multiple_of(owner * down_rows, down_rows), down_rows),
            pl.ds(pl.multiple_of(group * wide, wide), wide),
        ]

    def part(whole, owner):
        return whole.at[pl.ds(owner * local_experts, local_experts)]

    partner = (1 - g, f, t)
    keep = [
        pltpu.make_async_copy(part(gate, f), gate_at(gate_out, g, f), local_sem.at[0]),
        pltpu.make_async_copy(part(up, f), gate_at(up_out, g, f), local_sem.at[1]),
        pltpu.make_async_copy(normed, normed_all.at[f], local_sem.at[2]),
        pltpu.make_async_copy(routing, routing_all.at[f], local_sem.at[3]),
    ]
    main = {}
    for s in STEPS:
        there = flip(f, s)
        main[0, s] = remote(part(gate, there), gate_at(gate_out, g, f), send.at[0, s],
                            recv.at[0, s], (g, there, t))
        main[1, s] = remote(part(up, there), gate_at(up_out, g, f), send.at[1, s],
                            recv.at[1, s], (g, there, t))
        main[2, s] = remote(part(down, there), down_at(f, t), send.at[2, s], recv.at[2, s],
                            (t, there, g))
    turn = remote(part(down, f), down_at(f, t), send.at[2, 0], recv.at[2, 0], (1 - g, f, 1 - t))
    stay = pltpu.make_async_copy(part(down, f), down_at(f, t), local_sem.at[4])

    for s in STEPS:
        for which in range(3):
            main[which, s].start()

    @pl.when(g != t)
    def _():
        turn.start()

    @pl.when(g == t)
    def _():
        stay.start()

    for copy in keep:
        copy.start()

    relays = {}
    relays[0, 0] = remote(part(gate, f), gate_at(gate_out, g, f), relay_send.at[0, 0],
                          relay_recv.at[0, 0], partner)
    relays[1, 0] = remote(part(up, f), gate_at(up_out, g, f), relay_send.at[1, 0],
                          relay_recv.at[1, 0], partner)
    relays[0, 0].start()
    relays[1, 0].start()

    across = (g, flip(f, 1), t)
    second = {0: remote(own_half, tok(f), tok_send.at[1], tok_recv.at[1], across)}
    second[0].start()
    for s in (2, 4, 6):
        first[s].wait_recv()
        second[s] = remote(tok(flip(f, s)), tok(flip(f, s)), tok_send.at[s + 1],
                           tok_recv.at[s + 1], across)
        second[s].start()
    beside = (g, f, 1 - t)
    third = {}
    for s in (2, 4, 6, 1, 3, 5, 7):
        if s % 2:
            second[s - 1].wait_recv()
        third[s] = remote(tok(flip(f, s)), tok(flip(f, s)), tok_send.at[8 + s],
                          tok_recv.at[8 + s], beside)
        third[s].start()

    @pl.when(g != t)
    def _():
        turn.wait()

    @pl.when(g == t)
    def _():
        stay.wait()

    relays[2, 0] = remote(down_at(f, g), down_at(f, g), relay_send.at[2, 0],
                          relay_recv.at[2, 0], partner)
    relays[2, 0].start()
    for s in STEPS:
        source = flip(f, s)
        for which in range(3):
            main[which, s].wait_recv()
            if which == 2:
                block = down_at(source, g)
            else:
                block = gate_at((gate_out, up_out)[which], g, source)
            relays[which, s] = remote(block, block, relay_send.at[which, s],
                                      relay_recv.at[which, s], partner)
            relays[which, s].start()
    for s in (0,) + STEPS:
        for which in range(3):
            relays[which, s].wait()
    for s in STEPS:
        for which in range(3):
            main[which, s].wait_send()
        small[s].wait()
        third[s].wait()
    for s in (2, 4, 6):
        first[s].wait_send()
    for s in (0, 2, 4, 6):
        second[s].wait_send()
    for copy in keep:
        copy.wait()


def return_kernel(partial_mix, mixed, near, summed, far, send, recv, far_send, far_recv):
    g, f, t = lax.axis_index("gr"), lax.axis_index("fs"), lax.axis_index("tp")
    y = lax.rem(f, 2)
    half = mixed.shape[1]
    quad = ((0, 1), (1, 0), (1, 1))
    barrier = pltpu.get_barrier_semaphore()
    for dy, dx in quad:
        device = (g, flip(f, dy), 1 - t if dx else t)
        pl.semaphore_signal(barrier, inc=1, device_id=device, device_id_type=MESH)
    for step in (2, 4, 6):
        device = (g, flip(f, step), t)
        pl.semaphore_signal(barrier, inc=1, device_id=device, device_id_type=MESH)
    pl.semaphore_wait(barrier, 6)

    steps = (6, 4, 2, 0)
    copies = {}
    for i, step in enumerate(steps):
        for q, (dy, dx) in enumerate(quad):
            there = flip(f, step + dy)
            side = 1 - t if dx else t
            copies[i, q] = pltpu.make_async_remote_copy(
                src_ref=partial_mix.at[there, :, pl.ds(pl.multiple_of(side * half, half), half)],
                dst_ref=near.at[i, q],
                send_sem=send.at[i, q],
                recv_sem=recv.at[i, q],
                device_id=(g, flip(f, dy), side),
                device_id_type=MESH,
            )
            copies[i, q].start()
    onward = {}
    for i, step in enumerate(steps):
        for q in range(3):
            copies[i, q].wait_recv()
        there = flip(f, step)
        own = partial_mix[there, :, pl.ds(pl.multiple_of(t * half, half), half)]
        total = own.astype(jnp.float32)
        for q in range(3):
            total = total + near[i, q].astype(jnp.float32)
        if step:
            summed[i] = total.astype(jnp.bfloat16)
            onward[i] = pltpu.make_async_remote_copy(
                src_ref=summed.at[i],
                dst_ref=far.at[i],
                send_sem=far_send.at[i],
                recv_sem=far_recv.at[i],
                device_id=(g, there, t),
                device_id_type=MESH,
            )
            onward[i].start()
    for i in (2, 1, 0):
        onward[i].wait_recv()
        total = total + far[i].astype(jnp.float32)
    mixed[...] = total.astype(jnp.bfloat16)
    for i in range(3):
        onward[i].wait_send()
    for i in range(4):
        for q in range(3):
            copies[i, q].wait_send()


def body(tokens, norm_gain, gate_train, up_train, down_train, routes, route_weight):
    fs_n = 8
    experts, rows_in, hidden_part = gate_train.shape
    local_experts = experts // fs_n
    rows, width = tokens.shape
    top = routes.shape[1]
    gate_local = (norm_gain[None, :, None] * gate_train).astype(jnp.bfloat16)
    up_local = (norm_gain[None, :, None] * up_train).astype(jnp.bfloat16)
    down_local = down_train.astype(jnp.bfloat16)
    tokens_wide = tokens.astype(jnp.float32)
    normed = (
        tokens_wide
        * lax.rsqrt(jnp.mean(tokens_wide * tokens_wide, axis=1, keepdims=True) + NORM_EPSILON)
    ).astype(jnp.bfloat16)
    routing = jnp.concatenate([routes.astype(jnp.float32).T, route_weight.T], axis=0)

    anywhere = pl.BlockSpec(memory_space=pl.ANY)
    dma = pltpu.SemaphoreType.DMA
    normed_all, routing_all, gate_weight, up_weight, down_weight = pl.pallas_call(
        exchange_kernel,
        out_shape=(
            jax.ShapeDtypeStruct((fs_n, rows, width), jnp.bfloat16),
            jax.ShapeDtypeStruct((fs_n,) + routing.shape, jnp.float32),
            jax.ShapeDtypeStruct((local_experts, rows_in * 2 * fs_n, hidden_part), jnp.bfloat16),
            jax.ShapeDtypeStruct((local_experts, rows_in * 2 * fs_n, hidden_part), jnp.bfloat16),
            jax.ShapeDtypeStruct(
                (local_experts, down_train.shape[1] * fs_n, down_train.shape[2] * 2), jnp.bfloat16
            ),
        ),
        in_specs=[anywhere] * 5,
        out_specs=(anywhere,) * 5,
        scratch_shapes=[
            dma((3, 8)), dma((3, 8)), dma((3, 8)), dma((3, 8)), dma((5,)),
            dma((16,)), dma((16,)), dma((8,)), dma((8,)),
        ],
        compiler_params=pltpu.CompilerParams(collective_id=0, has_side_effects=True),
    )(normed, routing, gate_local, up_local, down_local)

    routes_all = routing_all[:, :top].astype(jnp.int32)
    weight_all = routing_all[:, top:]
    mine = lax.axis_index("fs") * local_experts + jnp.arange(local_experts, dtype=jnp.int32)
    hit = routes_all[:, None, :, :] == mine[None, :, None, None]
    chosen = jnp.any(hit, axis=2)
    share = jnp.sum(jnp.where(hit, weight_all[:, None, :, :], 0.0), axis=2)
    lower = (jnp.arange(rows)[:, None] <= jnp.arange(rows)[None, :]).astype(jnp.bfloat16)
    count = jnp.einsum(
        "bjt,ts->bjs", chosen.astype(jnp.bfloat16), lower, preferred_element_type=jnp.float32
    )
    slot = jnp.where(chosen, count.astype(jnp.int32) - 1, -1)
    place = slot[:, :, None, :] == jnp.arange(CAP, dtype=jnp.int32)[None, None, :, None]
    pick = place.astype(jnp.bfloat16).reshape(fs_n, local_experts * CAP, rows)
    spread = (
        jnp.where(place, share[:, :, None, :], 0.0)
        .astype(jnp.bfloat16)
        .reshape(fs_n, local_experts * CAP, rows)
    )
    arrived = jnp.einsum(
        "bst,btd->bsd", pick, normed_all, preferred_element_type=jnp.float32
    ).astype(jnp.bfloat16)
    arrived = (
        arrived.reshape(fs_n, local_experts, CAP, width)
        .transpose(1, 0, 2, 3)
        .reshape(local_experts, fs_n * CAP, width)
    )
    gate_pre = jnp.einsum("erd,edf->erf", arrived, gate_weight, preferred_element_type=jnp.float32)
    up_pre = jnp.einsum("erd,edf->erf", arrived, up_weight, preferred_element_type=jnp.float32)
    clipped = jnp.minimum(gate_pre, CLAMP_LIMIT)
    hidden = (
        (jnp.clip(up_pre, -CLAMP_LIMIT, CLAMP_LIMIT) + 1.0)
        * clipped
        * jax.nn.sigmoid(SLOPE_ALPHA * clipped)
    ).astype(jnp.bfloat16)
    results = jnp.einsum(
        "erf,efd->erd", hidden, down_weight, preferred_element_type=jnp.float32
    ).astype(jnp.bfloat16)
    results = (
        results.reshape(local_experts, fs_n, CAP, width)
        .transpose(1, 0, 2, 3)
        .reshape(fs_n, local_experts * CAP, width)
    )
    partial_mix = jnp.einsum(
        "bst,bsd->btd", spread, results, preferred_element_type=jnp.float32
    ).astype(jnp.bfloat16)

    in_vmem = pl.BlockSpec(memory_space=pltpu.VMEM)
    half = width // 2
    mixed = pl.pallas_call(
        return_kernel,
        out_shape=jax.ShapeDtypeStruct((rows, half), jnp.bfloat16),
        in_specs=[in_vmem],
        out_specs=in_vmem,
        scratch_shapes=[
            pltpu.VMEM((4, 3, rows, half), jnp.bfloat16),
            pltpu.VMEM((3, rows, half), jnp.bfloat16),
            pltpu.VMEM((3, rows, half), jnp.bfloat16),
            dma((4, 3)), dma((4, 3)), dma((3,)), dma((3,)),
        ],
        compiler_params=pltpu.CompilerParams(collective_id=1, has_side_effects=True),
    )(partial_mix)
    return (mixed, gate_weight, up_weight, down_weight)


def solution(mesh):
    placed = (
        P(("gr", "fs"), None),
        P(("gr", "fs")),
        P(None, ("gr", "fs"), "tp"),
        P(None, ("gr", "fs"), "tp"),
        P(None, ("gr", "fs"), "tp"),
        P(("gr", "fs"), None),
        P(("gr", "fs"), None),
    )
    block = mesh.shape["gr"] == 2 and mesh.shape["fs"] == 8 and mesh.shape["tp"] == 2
    return jax.shard_map(
        body if block else plain_body,
        mesh=mesh,
        in_specs=placed,
        out_specs=(
            P(("gr", "fs"), "tp"),
            P("fs", None, "tp"),
            P("fs", None, "tp"),
            P("fs", "tp", None),
        ),
        check_vma=False,
    )
```

```python
import jax
import jax.numpy as jnp
from jax import lax
from jax.experimental import pallas as pl
from jax.experimental.pallas import tpu as pltpu
from jax.sharding import PartitionSpec as P

EXPERTS = 32
TOP = 4
CAP = 32
CLAMP_LIMIT = 7.0
SLOPE_ALPHA = 1.702
NORM_EPSILON = 1e-06
MESH = pl.DeviceIdType.MESH
STEPS = (2, 3, 1, 6, 7, 4, 5)
OUTER = (2, 1, 3, 6, 7, 4, 5)
INNER = (6, 2, 7, 3, 4, 1, 5)


def plain_body(tokens, norm_gain, gate_train, up_train, down_train, routes, route_weight):
    gate_local = (norm_gain[None, :, None] * gate_train).astype(jnp.bfloat16)
    up_local = (norm_gain[None, :, None] * up_train).astype(jnp.bfloat16)
    down_local = down_train.astype(jnp.bfloat16)
    served = (
        lax.all_to_all(gate_local, "fs", split_axis=0, concat_axis=1, tiled=True),
        lax.all_to_all(up_local, "fs", split_axis=0, concat_axis=1, tiled=True),
        lax.all_to_all(down_local, "fs", split_axis=0, concat_axis=1, tiled=True),
    )
    gate_weight, up_weight, down_cols = (
        lax.all_gather(served[0], "gr", axis=1, tiled=True),
        lax.all_gather(served[1], "gr", axis=1, tiled=True),
        lax.all_gather(served[2], "gr", axis=1, tiled=True),
    )
    down_weight = lax.all_to_all(down_cols, "tp", split_axis=1, concat_axis=2, tiled=True)
    tokens_wide = tokens.astype(jnp.float32)
    normed = (
        tokens_wide
        * lax.rsqrt(jnp.mean(tokens_wide * tokens_wide, axis=1, keepdims=True) + NORM_EPSILON)
    ).astype(jnp.bfloat16)
    flat_routes = routes.reshape(-1)
    one_hot = (flat_routes[:, None] == jnp.arange(EXPERTS, dtype=jnp.int32)[None, :]).astype(
        jnp.int32
    )
    counts = jnp.cumsum(one_hot, axis=0)
    slot_index = jnp.sum((counts - 1) * one_hot, axis=1)
    target_rows = flat_routes * CAP + slot_index
    copied_rows = jnp.repeat(normed, TOP, axis=0)
    dispatch_buffer = (
        jnp.zeros((EXPERTS * CAP, normed.shape[1]), jnp.bfloat16).at[target_rows].set(copied_rows)
    )
    dispatch_buffer = dispatch_buffer.reshape(EXPERTS, CAP, normed.shape[1])
    arrived = lax.all_to_all(dispatch_buffer, "fs", split_axis=0, concat_axis=1, tiled=True)
    gate_pre = jnp.einsum("erd,edf->erf", arrived, gate_weight, preferred_element_type=jnp.float32)
    up_pre = jnp.einsum("erd,edf->erf", arrived, up_weight, preferred_element_type=jnp.float32)
    clipped = jnp.minimum(gate_pre, CLAMP_LIMIT)
    hidden = (
        (jnp.clip(up_pre, -CLAMP_LIMIT, CLAMP_LIMIT) + 1.0)
        * clipped
        * jax.nn.sigmoid(SLOPE_ALPHA * clipped)
    ).astype(jnp.bfloat16)
    partial_value = jnp.einsum(
        "erf,efd->erd", hidden, down_weight, preferred_element_type=jnp.float32
    )
    summed = lax.psum_scatter(
        partial_value.astype(jnp.bfloat16), "tp", scatter_dimension=2, tiled=True
    )
    returned = lax.all_to_all(summed, "fs", split_axis=1, concat_axis=0, tiled=True)
    features = returned.shape[2]
    picked = (
        returned.reshape(EXPERTS * CAP, features)[target_rows]
        .reshape(tokens.shape[0], TOP, features)
        .astype(jnp.float32)
    )
    mixed = jnp.sum(picked * route_weight[:, :, None], axis=1).astype(jnp.bfloat16)
    return (mixed, gate_weight, up_weight, down_weight)


def flip(fs, step):
    z, y = lax.div(fs, 2), lax.rem(fs, 2)
    turn = lax.div(step, 2) if not isinstance(step, int) else step // 2
    low = lax.rem(lax.rem(z, 2) + turn, 2)
    high = lax.rem(lax.div(z, 2) + (turn // 2 if isinstance(turn, int) else lax.div(turn, 2)), 2)
    return (high * 2 + low) * 2 + lax.rem(y + step, 2)


def exchange_kernel(
    normed, routing, gain, gate, up, down,
    normed_all, routing_all, gate_out, up_out, down_out,
    gate_half, up_half, down_half, gate_stage, up_stage, down_stage, load_sem,
    send, recv, relay_send, relay_recv, local_sem, tok_send, tok_recv, route_send, route_recv,
):
    g, f, t = lax.axis_index("gr"), lax.axis_index("fs"), lax.axis_index("tp")
    local_experts = gate_out.shape[0]
    fs_n = 8
    rows, down_rows = gate.shape[1], down.shape[1]
    wide = down.shape[2]
    half = normed.shape[1] // 2

    barrier = pltpu.get_barrier_semaphore()

    def greet(device):
        pl.semaphore_signal(barrier, inc=1, device_id=device, device_id_type=MESH)

    for step in STEPS:
        greet((g, flip(f, step), t))
    for step in range(fs_n):
        greet((1 - g, flip(f, step), 1 - t))
    greet((1 - g, f, t))
    greet((g, f, 1 - t))
    pl.semaphore_wait(barrier, 17)

    def remote(src, dst, s, r, device):
        return pltpu.make_async_remote_copy(
            src_ref=src, dst_ref=dst, send_sem=s, recv_sem=r, device_id=device, device_id_type=MESH
        )

    def tok(block):
        return normed_all.at[block, :, pl.ds(pl.multiple_of(t * half, half), half)]

    own_half = normed.at[:, pl.ds(pl.multiple_of(t * half, half), half)]
    first = {s: remote(own_half, tok(f), tok_send.at[s], tok_recv.at[s], (g, flip(f, s), t))
             for s in (2, 4, 6)}
    for s in (6, 4, 2):
        first[s].start()
    small = {s: remote(routing, routing_all.at[f], route_send.at[s], route_recv.at[s],
                       (g, flip(f, s), t)) for s in STEPS}
    for s in STEPS:
        small[s].start()

    def gate_at(whole, group, owner):
        return whole.at[:, pl.ds(pl.multiple_of((group * fs_n + owner) * rows, rows), rows), :]

    def down_at(owner, group):
        return down_out.at[
            :,
            pl.ds(pl.multiple_of(owner * down_rows, down_rows), down_rows),
            pl.ds(pl.multiple_of(group * wide, wide), wide),
        ]

    def part(whole, owner):
        return whole.at[pl.ds(owner * local_experts, local_experts)]

    partner = (1 - g, f, t)
    keep = [
        pltpu.make_async_copy(normed, normed_all.at[f], local_sem.at[2]),
        pltpu.make_async_copy(routing, routing_all.at[f], local_sem.at[3]),
    ]
    for copy in keep:
        copy.start()

    inner = lax.rem(lax.div(lax.div(f, 2) + 1, 2), 2)
    order = [a + inner * (b - a) for a, b in zip(OUTER, INNER)] + [0]
    stages, halves = (gate_stage, up_stage, down_stage), (gate_half, up_half, down_half)

    def load(position, which):
        there = flip(f, order[position])
        return pltpu.make_async_copy(
            part((gate, up, down)[which], there),
            stages[which].at[position % 2],
            load_sem.at[which, position % 2],
        )

    main = {}
    relays = {}
    for which in range(3):
        load(0, which).start()
    for position, step in enumerate(order):
        there = flip(f, step)
        for which in range(3):
            if position + 1 < len(order):
                load(position + 1, which).start()
            load(position, which).wait()
            stage, halved = stages[which], halves[which]

            @pl.loop(0, local_experts)
            def _(e):
                wide_block = stage[position % 2, e]
                if which < 2:
                    wide_block = gain[...] * wide_block
                halved[position, e] = wide_block.astype(jnp.bfloat16)

            if position + 1 < len(order):
                target = (t, there, g) if which == 2 else (g, there, t)
                place = down_at(f, t) if which == 2 else gate_at((gate_out, up_out)[which], g, f)
                main[which, position] = remote(
                    halved.at[position], place, send.at[which, step], recv.at[which, step], target
                )
                main[which, position].start()
    last = len(order) - 1
    turn = remote(down_half.at[last], down_at(f, t), send.at[2, 0], recv.at[2, 0],
                  (1 - g, f, 1 - t))
    stay = pltpu.make_async_copy(down_half.at[last], down_at(f, t), local_sem.at[4])

    @pl.when(g != t)
    def _():
        turn.start()

    @pl.when(g == t)
    def _():
        stay.start()

    for which in range(2):
        place = gate_at((gate_out, up_out)[which], g, f)
        keep.append(pltpu.make_async_copy(halves[which].at[last], place, local_sem.at[which]))
        keep[-1].start()
        relays[which, 0] = remote(halves[which].at[last], place, relay_send.at[which, 0],
                                  relay_recv.at[which, 0], partner)
        relays[which, 0].start()

    across = (g, flip(f, 1), t)
    second = {0: remote(own_half, tok(f), tok_send.at[1], tok_recv.at[1], across)}
    second[0].start()
    for s in (2, 4, 6):
        first[s].wait_recv()
        second[s] = remote(tok(flip(f, s)), tok(flip(f, s)), tok_send.at[s + 1],
                           tok_recv.at[s + 1], across)
        second[s].start()
    beside = (g, f, 1 - t)
    third = {}
    for s in (2, 4, 6, 1, 3, 5, 7):
        if s % 2:
            second[s - 1].wait_recv()
        third[s] = remote(tok(flip(f, s)), tok(flip(f, s)), tok_send.at[8 + s],
                          tok_recv.at[8 + s], beside)
        third[s].start()

    @pl.when(g != t)
    def _():
        turn.wait()

    @pl.when(g == t)
    def _():
        stay.wait()

    relays[2, 0] = remote(down_at(f, g), down_at(f, g), relay_send.at[2, 0],
                          relay_recv.at[2, 0], partner)
    relays[2, 0].start()
    for s in STEPS:
        source = flip(f, s)
        for which in range(3):
            if which == 2:
                block = down_at(source, g)
            else:
                block = gate_at((gate_out, up_out)[which], g, source)
            remote(halves[which].at[0], block, send.at[which, s], recv.at[which, s],
                   partner).wait_recv()
            relays[which, s] = remote(block, block, relay_send.at[which, s],
                                      relay_recv.at[which, s], partner)
            relays[which, s].start()
    for s in (0,) + STEPS:
        for which in range(3):
            relays[which, s].wait()
    for copy in main.values():
        copy.wait_send()
    for s in STEPS:
        small[s].wait()
        third[s].wait()
    for s in (2, 4, 6):
        first[s].wait_send()
    for s in (0, 2, 4, 6):
        second[s].wait_send()
    for copy in keep:
        copy.wait()


def return_kernel(partial_mix, mixed, near, summed, far, send, recv, far_send, far_recv):
    g, f, t = lax.axis_index("gr"), lax.axis_index("fs"), lax.axis_index("tp")
    y = lax.rem(f, 2)
    half = mixed.shape[1]
    quad = ((0, 1), (1, 0), (1, 1))
    barrier = pltpu.get_barrier_semaphore()
    for dy, dx in quad:
        device = (g, flip(f, dy), 1 - t if dx else t)
        pl.semaphore_signal(barrier, inc=1, device_id=device, device_id_type=MESH)
    for step in (2, 4, 6):
        device = (g, flip(f, step), t)
        pl.semaphore_signal(barrier, inc=1, device_id=device, device_id_type=MESH)
    pl.semaphore_wait(barrier, 6)

    steps = (6, 4, 2, 0)
    copies = {}
    for i, step in enumerate(steps):
        for q, (dy, dx) in enumerate(quad):
            there = flip(f, step + dy)
            side = 1 - t if dx else t
            copies[i, q] = pltpu.make_async_remote_copy(
                src_ref=partial_mix.at[there, :, pl.ds(pl.multiple_of(side * half, half), half)],
                dst_ref=near.at[i, q],
                send_sem=send.at[i, q],
                recv_sem=recv.at[i, q],
                device_id=(g, flip(f, dy), side),
                device_id_type=MESH,
            )
            copies[i, q].start()
    onward = {}
    for i, step in enumerate(steps):
        for q in range(3):
            copies[i, q].wait_recv()
        there = flip(f, step)
        own = partial_mix[there, :, pl.ds(pl.multiple_of(t * half, half), half)]
        total = own.astype(jnp.float32)
        for q in range(3):
            total = total + near[i, q].astype(jnp.float32)
        if step:
            summed[i] = total.astype(jnp.bfloat16)
            onward[i] = pltpu.make_async_remote_copy(
                src_ref=summed.at[i],
                dst_ref=far.at[i],
                send_sem=far_send.at[i],
                recv_sem=far_recv.at[i],
                device_id=(g, there, t),
                device_id_type=MESH,
            )
            onward[i].start()
    for i in (2, 1, 0):
        onward[i].wait_recv()
        total = total + far[i].astype(jnp.float32)
    mixed[...] = total.astype(jnp.bfloat16)
    for i in range(3):
        onward[i].wait_send()
    for i in range(4):
        for q in range(3):
            copies[i, q].wait_send()


def expert_kernel(arrived, gate, up, down, results, gate_out, up_out, down_out):
    gate_out[...] = gate[...]
    up_out[...] = up[...]
    down_out[...] = down[...]
    rows = arrived[...]
    gate_pre = jnp.dot(rows, gate[...], preferred_element_type=jnp.float32)
    up_pre = jnp.dot(rows, up[...], preferred_element_type=jnp.float32)
    clipped = jnp.minimum(gate_pre, CLAMP_LIMIT)
    hidden = (
        (jnp.clip(up_pre, -CLAMP_LIMIT, CLAMP_LIMIT) + 1.0)
        * clipped
        * jax.nn.sigmoid(SLOPE_ALPHA * clipped)
    ).astype(jnp.bfloat16)
    results[...] = jnp.dot(hidden, down[...], preferred_element_type=jnp.float32).astype(
        jnp.bfloat16
    )


def body(tokens, norm_gain, gate_train, up_train, down_train, routes, route_weight):
    fs_n = 8
    experts, rows_in, hidden_part = gate_train.shape
    local_experts = experts // fs_n
    rows, width = tokens.shape
    top = routes.shape[1]
    gain = jnp.broadcast_to(norm_gain[:, None], (rows_in, hidden_part))
    tokens_wide = tokens.astype(jnp.float32)
    normed = (
        tokens_wide
        * lax.rsqrt(jnp.mean(tokens_wide * tokens_wide, axis=1, keepdims=True) + NORM_EPSILON)
    ).astype(jnp.bfloat16)
    routing = jnp.concatenate([routes.astype(jnp.float32).T, route_weight.T], axis=0)

    anywhere = pl.BlockSpec(memory_space=pl.ANY)
    dma = pltpu.SemaphoreType.DMA
    normed_all, routing_all, gate_weight, up_weight, down_weight = pl.pallas_call(
        exchange_kernel,
        out_shape=(
            jax.ShapeDtypeStruct((fs_n, rows, width), jnp.bfloat16),
            jax.ShapeDtypeStruct((fs_n,) + routing.shape, jnp.float32),
            jax.ShapeDtypeStruct((local_experts, rows_in * 2 * fs_n, hidden_part), jnp.bfloat16),
            jax.ShapeDtypeStruct((local_experts, rows_in * 2 * fs_n, hidden_part), jnp.bfloat16),
            jax.ShapeDtypeStruct(
                (local_experts, down_train.shape[1] * fs_n, down_train.shape[2] * 2), jnp.bfloat16
            ),
        ),
        in_specs=[anywhere] * 2 + [pl.BlockSpec(memory_space=pltpu.VMEM)] + [anywhere] * 3,
        out_specs=(anywhere,) * 5,
        scratch_shapes=[
            pltpu.VMEM((fs_n, local_experts) + gate_train.shape[1:], jnp.bfloat16),
            pltpu.VMEM((fs_n, local_experts) + up_train.shape[1:], jnp.bfloat16),
            pltpu.VMEM((fs_n, local_experts) + down_train.shape[1:], jnp.bfloat16),
            pltpu.VMEM((2, local_experts) + gate_train.shape[1:], jnp.float32),
            pltpu.VMEM((2, local_experts) + up_train.shape[1:], jnp.float32),
            pltpu.VMEM((2, local_experts) + down_train.shape[1:], jnp.float32),
            dma((3, 2)),
            dma((3, 8)), dma((3, 8)), dma((3, 8)), dma((3, 8)), dma((5,)),
            dma((16,)), dma((16,)), dma((8,)), dma((8,)),
        ],
        compiler_params=pltpu.CompilerParams(collective_id=0, has_side_effects=True),
    )(normed, routing, gain, gate_train, up_train, down_train)

    routes_all = routing_all[:, :top].astype(jnp.int32)
    weight_all = routing_all[:, top:]
    mine = lax.axis_index("fs") * local_experts + jnp.arange(local_experts, dtype=jnp.int32)
    hit = routes_all[:, None, :, :] == mine[None, :, None, None]
    chosen = jnp.any(hit, axis=2)
    share = jnp.sum(jnp.where(hit, weight_all[:, None, :, :], 0.0), axis=2)
    lower = (jnp.arange(rows)[:, None] <= jnp.arange(rows)[None, :]).astype(jnp.bfloat16)
    count = jnp.einsum(
        "bjt,ts->bjs", chosen.astype(jnp.bfloat16), lower, preferred_element_type=jnp.float32
    )
    slot = jnp.where(chosen, count.astype(jnp.int32) - 1, -1)
    place = slot[:, :, None, :] == jnp.arange(CAP, dtype=jnp.int32)[None, None, :, None]
    pick = place.astype(jnp.bfloat16).reshape(fs_n, local_experts * CAP, rows)
    spread = (
        jnp.where(place, share[:, :, None, :], 0.0)
        .astype(jnp.bfloat16)
        .reshape(fs_n, local_experts * CAP, rows)
    )
    arrived = jnp.einsum(
        "bst,btd->bsd", pick, normed_all, preferred_element_type=jnp.float32
    ).astype(jnp.bfloat16)
    arrived = (
        arrived.reshape(fs_n, local_experts, CAP, width)
        .transpose(1, 0, 2, 3)
        .reshape(local_experts, fs_n * CAP, width)
    )
    def block(array):
        return pl.BlockSpec((None,) + array.shape[1:], lambda e: (e, 0, 0))

    weights = (gate_weight, up_weight, down_weight)
    results, gate_weight, up_weight, down_weight = pl.pallas_call(
        expert_kernel,
        grid=(local_experts,),
        out_shape=[jax.ShapeDtypeStruct(a.shape, jnp.bfloat16) for a in (arrived,) + weights],
        in_specs=[block(a) for a in (arrived,) + weights],
        out_specs=[block(a) for a in (arrived,) + weights],
    )(arrived, *weights)
    results = (
        results.reshape(local_experts, fs_n, CAP, width)
        .transpose(1, 0, 2, 3)
        .reshape(fs_n, local_experts * CAP, width)
    )
    partial_mix = jnp.einsum(
        "bst,bsd->btd", spread, results, preferred_element_type=jnp.float32
    ).astype(jnp.bfloat16)

    in_vmem = pl.BlockSpec(memory_space=pltpu.VMEM)
    half = width // 2
    mixed = pl.pallas_call(
        return_kernel,
        out_shape=jax.ShapeDtypeStruct((rows, half), jnp.bfloat16),
        in_specs=[in_vmem],
        out_specs=in_vmem,
        scratch_shapes=[
            pltpu.VMEM((4, 3, rows, half), jnp.bfloat16),
            pltpu.VMEM((3, rows, half), jnp.bfloat16),
            pltpu.VMEM((3, rows, half), jnp.bfloat16),
            dma((4, 3)), dma((4, 3)), dma((3,)), dma((3,)),
        ],
        compiler_params=pltpu.CompilerParams(collective_id=1, has_side_effects=True),
    )(partial_mix)
    return (mixed, gate_weight, up_weight, down_weight)


def solution(mesh):
    placed = (
        P(("gr", "fs"), None),
        P(("gr", "fs")),
        P(None, ("gr", "fs"), "tp"),
        P(None, ("gr", "fs"), "tp"),
        P(None, ("gr", "fs"), "tp"),
        P(("gr", "fs"), None),
        P(("gr", "fs"), None),
    )
    block = mesh.shape["gr"] == 2 and mesh.shape["fs"] == 8 and mesh.shape["tp"] == 2
    return jax.shard_map(
        body if block else plain_body,
        mesh=mesh,
        in_specs=placed,
        out_specs=(
            P(("gr", "fs"), "tp"),
            P("fs", None, "tp"),
            P("fs", None, "tp"),
            P("fs", "tp", None),
        ),
        check_vma=False,
    )
```

```python
import jax
import jax.numpy as jnp
from jax import lax
from jax.experimental import pallas as pl
from jax.experimental.pallas import tpu as pltpu
from jax.sharding import PartitionSpec as P

EXPERTS = 32
TOP = 4
CAP = 32
CLAMP_LIMIT = 7.0
SLOPE_ALPHA = 1.702
NORM_EPSILON = 1e-06
MESH = pl.DeviceIdType.MESH
STEPS = (2, 3, 1, 6, 7, 4, 5)
OUTER = (6, 2, 7, 3, 4, 1, 5)
INNER = (4, 2, 5, 3, 6, 1, 7)


def plain_body(tokens, norm_gain, gate_train, up_train, down_train, routes, route_weight):
    gate_local = (norm_gain[None, :, None] * gate_train).astype(jnp.bfloat16)
    up_local = (norm_gain[None, :, None] * up_train).astype(jnp.bfloat16)
    down_local = down_train.astype(jnp.bfloat16)
    served = (
        lax.all_to_all(gate_local, "fs", split_axis=0, concat_axis=1, tiled=True),
        lax.all_to_all(up_local, "fs", split_axis=0, concat_axis=1, tiled=True),
        lax.all_to_all(down_local, "fs", split_axis=0, concat_axis=1, tiled=True),
    )
    gate_weight, up_weight, down_cols = (
        lax.all_gather(served[0], "gr", axis=1, tiled=True),
        lax.all_gather(served[1], "gr", axis=1, tiled=True),
        lax.all_gather(served[2], "gr", axis=1, tiled=True),
    )
    down_weight = lax.all_to_all(down_cols, "tp", split_axis=1, concat_axis=2, tiled=True)
    tokens_wide = tokens.astype(jnp.float32)
    normed = (
        tokens_wide
        * lax.rsqrt(jnp.mean(tokens_wide * tokens_wide, axis=1, keepdims=True) + NORM_EPSILON)
    ).astype(jnp.bfloat16)
    flat_routes = routes.reshape(-1)
    one_hot = (flat_routes[:, None] == jnp.arange(EXPERTS, dtype=jnp.int32)[None, :]).astype(
        jnp.int32
    )
    counts = jnp.cumsum(one_hot, axis=0)
    slot_index = jnp.sum((counts - 1) * one_hot, axis=1)
    target_rows = flat_routes * CAP + slot_index
    copied_rows = jnp.repeat(normed, TOP, axis=0)
    dispatch_buffer = (
        jnp.zeros((EXPERTS * CAP, normed.shape[1]), jnp.bfloat16).at[target_rows].set(copied_rows)
    )
    dispatch_buffer = dispatch_buffer.reshape(EXPERTS, CAP, normed.shape[1])
    arrived = lax.all_to_all(dispatch_buffer, "fs", split_axis=0, concat_axis=1, tiled=True)
    gate_pre = jnp.einsum("erd,edf->erf", arrived, gate_weight, preferred_element_type=jnp.float32)
    up_pre = jnp.einsum("erd,edf->erf", arrived, up_weight, preferred_element_type=jnp.float32)
    clipped = jnp.minimum(gate_pre, CLAMP_LIMIT)
    hidden = (
        (jnp.clip(up_pre, -CLAMP_LIMIT, CLAMP_LIMIT) + 1.0)
        * clipped
        * jax.nn.sigmoid(SLOPE_ALPHA * clipped)
    ).astype(jnp.bfloat16)
    partial_value = jnp.einsum(
        "erf,efd->erd", hidden, down_weight, preferred_element_type=jnp.float32
    )
    summed = lax.psum_scatter(
        partial_value.astype(jnp.bfloat16), "tp", scatter_dimension=2, tiled=True
    )
    returned = lax.all_to_all(summed, "fs", split_axis=1, concat_axis=0, tiled=True)
    features = returned.shape[2]
    picked = (
        returned.reshape(EXPERTS * CAP, features)[target_rows]
        .reshape(tokens.shape[0], TOP, features)
        .astype(jnp.float32)
    )
    mixed = jnp.sum(picked * route_weight[:, :, None], axis=1).astype(jnp.bfloat16)
    return (mixed, gate_weight, up_weight, down_weight)


def flip(fs, step):
    z, y = lax.div(fs, 2), lax.rem(fs, 2)
    turn = lax.div(step, 2) if not isinstance(step, int) else step // 2
    low = lax.rem(lax.rem(z, 2) + turn, 2)
    high = lax.rem(lax.div(z, 2) + (turn // 2 if isinstance(turn, int) else lax.div(turn, 2)), 2)
    return (high * 2 + low) * 2 + lax.rem(y + step, 2)


def exchange_kernel(
    normed, routing, gain, gate, up, down,
    normed_all, routing_all, gate_out, up_out, down_out,
    gate_half, up_half, down_half, gate_stage, up_stage, down_stage, load_sem,
    send, recv, relay_send, relay_recv, local_sem, tok_send, tok_recv, route_send, route_recv,
):
    g, f, t = lax.axis_index("gr"), lax.axis_index("fs"), lax.axis_index("tp")
    local_experts = gate_out.shape[0]
    fs_n = 8
    rows, down_rows = gate.shape[1], down.shape[1]
    wide = down.shape[2]
    half = normed.shape[1] // 2

    barrier = pltpu.get_barrier_semaphore()

    def greet(device):
        pl.semaphore_signal(barrier, inc=1, device_id=device, device_id_type=MESH)

    for step in STEPS:
        greet((g, flip(f, step), t))
    for step in range(fs_n):
        greet((1 - g, flip(f, step), 1 - t))
    greet((1 - g, f, t))
    greet((g, f, 1 - t))
    pl.semaphore_wait(barrier, 17)

    def remote(src, dst, s, r, device):
        return pltpu.make_async_remote_copy(
            src_ref=src, dst_ref=dst, send_sem=s, recv_sem=r, device_id=device, device_id_type=MESH
        )

    def tok(block):
        return normed_all.at[block, :, pl.ds(pl.multiple_of(t * half, half), half)]

    own_half = normed.at[:, pl.ds(pl.multiple_of(t * half, half), half)]
    first = {s: remote(own_half, tok(f), tok_send.at[s], tok_recv.at[s], (g, flip(f, s), t))
             for s in (2, 4, 6)}
    for s in (6, 4, 2):
        first[s].start()
    small = {s: remote(routing, routing_all.at[f], route_send.at[s], route_recv.at[s],
                       (g, flip(f, s), t)) for s in STEPS}
    for s in STEPS:
        small[s].start()

    def gate_at(whole, group, owner):
        return whole.at[:, pl.ds(pl.multiple_of((group * fs_n + owner) * rows, rows), rows), :]

    def down_at(owner, group):
        return down_out.at[
            :,
            pl.ds(pl.multiple_of(owner * down_rows, down_rows), down_rows),
            pl.ds(pl.multiple_of(group * wide, wide), wide),
        ]

    def part(whole, owner):
        return whole.at[pl.ds(owner * local_experts, local_experts)]

    partner = (1 - g, f, t)
    keep = [
        pltpu.make_async_copy(normed, normed_all.at[f], local_sem.at[2]),
        pltpu.make_async_copy(routing, routing_all.at[f], local_sem.at[3]),
    ]
    for copy in keep:
        copy.start()

    inner = lax.rem(lax.div(lax.div(f, 2) + 1, 2), 2)
    order = [a + inner * (b - a) for a, b in zip(OUTER, INNER)] + [0]
    stages, halves = (gate_stage, up_stage, down_stage), (gate_half, up_half, down_half)

    def load(position, which):
        there = flip(f, order[position])
        return pltpu.make_async_copy(
            part((gate, up, down)[which], there),
            stages[which].at[position % 2],
            load_sem.at[which, position % 2],
        )

    main = {}
    relays = {}
    for which in range(3):
        load(0, which).start()
    for position, step in enumerate(order):
        there = flip(f, step)
        for which in range(3):
            if position + 1 < len(order):
                load(position + 1, which).start()
            load(position, which).wait()
            stage, halved = stages[which], halves[which]

            @pl.loop(0, local_experts)
            def _(e):
                wide_block = stage[position % 2, e]
                if which < 2:
                    wide_block = gain[...] * wide_block
                halved[position, e] = wide_block.astype(jnp.bfloat16)

            if position + 1 < len(order):
                target = (t, there, g) if which == 2 else (g, there, t)
                place = down_at(f, t) if which == 2 else gate_at((gate_out, up_out)[which], g, f)
                main[which, position] = remote(
                    halved.at[position], place, send.at[which, step], recv.at[which, step], target
                )
                main[which, position].start()
    last = len(order) - 1
    turn = remote(down_half.at[last], down_at(f, t), send.at[2, 0], recv.at[2, 0],
                  (1 - g, f, 1 - t))
    stay = pltpu.make_async_copy(down_half.at[last], down_at(f, t), local_sem.at[4])

    @pl.when(g != t)
    def _():
        turn.start()

    @pl.when(g == t)
    def _():
        stay.start()

    for which in range(2):
        place = gate_at((gate_out, up_out)[which], g, f)
        keep.append(pltpu.make_async_copy(halves[which].at[last], place, local_sem.at[which]))
        keep[-1].start()
        relays[which, 0] = remote(halves[which].at[last], place, relay_send.at[which, 0],
                                  relay_recv.at[which, 0], partner)
        relays[which, 0].start()

    across = (g, flip(f, 1), t)
    second = {0: remote(own_half, tok(f), tok_send.at[1], tok_recv.at[1], across)}
    second[0].start()
    for s in (2, 4, 6):
        first[s].wait_recv()
        second[s] = remote(tok(flip(f, s)), tok(flip(f, s)), tok_send.at[s + 1],
                           tok_recv.at[s + 1], across)
        second[s].start()
    beside = (g, f, 1 - t)
    third = {}
    for s in (2, 4, 6, 1, 3, 5, 7):
        if s % 2:
            second[s - 1].wait_recv()
        third[s] = remote(tok(flip(f, s)), tok(flip(f, s)), tok_send.at[8 + s],
                          tok_recv.at[8 + s], beside)
        third[s].start()

    @pl.when(g != t)
    def _():
        turn.wait()

    @pl.when(g == t)
    def _():
        stay.wait()

    relays[2, 0] = remote(down_at(f, g), down_at(f, g), relay_send.at[2, 0],
                          relay_recv.at[2, 0], partner)
    relays[2, 0].start()
    for s in STEPS:
        source = flip(f, s)
        for which in range(3):
            if which == 2:
                block = down_at(source, g)
            else:
                block = gate_at((gate_out, up_out)[which], g, source)
            remote(halves[which].at[0], block, send.at[which, s], recv.at[which, s],
                   partner).wait_recv()
            relays[which, s] = remote(block, block, relay_send.at[which, s],
                                      relay_recv.at[which, s], partner)
            relays[which, s].start()
    for s in (0,) + STEPS:
        for which in range(3):
            relays[which, s].wait()
    for copy in main.values():
        copy.wait_send()
    for s in STEPS:
        small[s].wait()
        third[s].wait()
    for s in (2, 4, 6):
        first[s].wait_send()
    for s in (0, 2, 4, 6):
        second[s].wait_send()
    for copy in keep:
        copy.wait()


def return_kernel(partial_mix, mixed, near, summed, far, send, recv, far_send, far_recv):
    g, f, t = lax.axis_index("gr"), lax.axis_index("fs"), lax.axis_index("tp")
    y = lax.rem(f, 2)
    half = mixed.shape[1]
    quad = ((0, 1), (1, 0), (1, 1))
    barrier = pltpu.get_barrier_semaphore()
    for dy, dx in quad:
        device = (g, flip(f, dy), 1 - t if dx else t)
        pl.semaphore_signal(barrier, inc=1, device_id=device, device_id_type=MESH)
    for step in (2, 4, 6):
        device = (g, flip(f, step), t)
        pl.semaphore_signal(barrier, inc=1, device_id=device, device_id_type=MESH)
    pl.semaphore_wait(barrier, 6)

    steps = (6, 4, 2, 0)
    copies = {}
    for i, step in enumerate(steps):
        for q, (dy, dx) in enumerate(quad):
            there = flip(f, step + dy)
            side = 1 - t if dx else t
            copies[i, q] = pltpu.make_async_remote_copy(
                src_ref=partial_mix.at[there, :, pl.ds(pl.multiple_of(side * half, half), half)],
                dst_ref=near.at[i, q],
                send_sem=send.at[i, q],
                recv_sem=recv.at[i, q],
                device_id=(g, flip(f, dy), side),
                device_id_type=MESH,
            )
            copies[i, q].start()
    onward = {}
    for i, step in enumerate(steps):
        for q in range(3):
            copies[i, q].wait_recv()
        there = flip(f, step)
        own = partial_mix[there, :, pl.ds(pl.multiple_of(t * half, half), half)]
        total = own.astype(jnp.float32)
        for q in range(3):
            total = total + near[i, q].astype(jnp.float32)
        if step:
            summed[i] = total.astype(jnp.bfloat16)
            onward[i] = pltpu.make_async_remote_copy(
                src_ref=summed.at[i],
                dst_ref=far.at[i],
                send_sem=far_send.at[i],
                recv_sem=far_recv.at[i],
                device_id=(g, there, t),
                device_id_type=MESH,
            )
            onward[i].start()
    for i in (2, 1, 0):
        onward[i].wait_recv()
        total = total + far[i].astype(jnp.float32)
    mixed[...] = total.astype(jnp.bfloat16)
    for i in range(3):
        onward[i].wait_send()
    for i in range(4):
        for q in range(3):
            copies[i, q].wait_send()


def expert_kernel(arrived, gate, up, down, results, gate_out, up_out, down_out):
    gate_out[...] = gate[...]
    up_out[...] = up[...]
    down_out[...] = down[...]
    rows = arrived[...]
    gate_pre = jnp.dot(rows, gate[...], preferred_element_type=jnp.float32)
    up_pre = jnp.dot(rows, up[...], preferred_element_type=jnp.float32)
    clipped = jnp.minimum(gate_pre, CLAMP_LIMIT)
    hidden = (
        (jnp.clip(up_pre, -CLAMP_LIMIT, CLAMP_LIMIT) + 1.0)
        * clipped
        * jax.nn.sigmoid(SLOPE_ALPHA * clipped)
    ).astype(jnp.bfloat16)
    results[...] = jnp.dot(hidden, down[...], preferred_element_type=jnp.float32).astype(
        jnp.bfloat16
    )


def body(tokens, norm_gain, gate_train, up_train, down_train, routes, route_weight):
    fs_n = 8
    experts, rows_in, hidden_part = gate_train.shape
    local_experts = experts // fs_n
    rows, width = tokens.shape
    top = routes.shape[1]
    gain = jnp.broadcast_to(norm_gain[:, None], (rows_in, hidden_part))
    tokens_wide = tokens.astype(jnp.float32)
    normed = (
        tokens_wide
        * lax.rsqrt(jnp.mean(tokens_wide * tokens_wide, axis=1, keepdims=True) + NORM_EPSILON)
    ).astype(jnp.bfloat16)
    routing = jnp.concatenate([routes.astype(jnp.float32).T, route_weight.T], axis=0)

    anywhere = pl.BlockSpec(memory_space=pl.ANY)
    dma = pltpu.SemaphoreType.DMA
    normed_all, routing_all, gate_weight, up_weight, down_weight = pl.pallas_call(
        exchange_kernel,
        out_shape=(
            jax.ShapeDtypeStruct((fs_n, rows, width), jnp.bfloat16),
            jax.ShapeDtypeStruct((fs_n,) + routing.shape, jnp.float32),
            jax.ShapeDtypeStruct((local_experts, rows_in * 2 * fs_n, hidden_part), jnp.bfloat16),
            jax.ShapeDtypeStruct((local_experts, rows_in * 2 * fs_n, hidden_part), jnp.bfloat16),
            jax.ShapeDtypeStruct(
                (local_experts, down_train.shape[1] * fs_n, down_train.shape[2] * 2), jnp.bfloat16
            ),
        ),
        in_specs=[anywhere] * 2 + [pl.BlockSpec(memory_space=pltpu.VMEM)] + [anywhere] * 3,
        out_specs=(anywhere,) * 5,
        scratch_shapes=[
            pltpu.VMEM((fs_n, local_experts) + gate_train.shape[1:], jnp.bfloat16),
            pltpu.VMEM((fs_n, local_experts) + up_train.shape[1:], jnp.bfloat16),
            pltpu.VMEM((fs_n, local_experts) + down_train.shape[1:], jnp.bfloat16),
            pltpu.VMEM((2, local_experts) + gate_train.shape[1:], jnp.float32),
            pltpu.VMEM((2, local_experts) + up_train.shape[1:], jnp.float32),
            pltpu.VMEM((2, local_experts) + down_train.shape[1:], jnp.float32),
            dma((3, 2)),
            dma((3, 8)), dma((3, 8)), dma((3, 8)), dma((3, 8)), dma((5,)),
            dma((16,)), dma((16,)), dma((8,)), dma((8,)),
        ],
        compiler_params=pltpu.CompilerParams(collective_id=0, has_side_effects=True),
    )(normed, routing, gain, gate_train, up_train, down_train)

    routes_all = routing_all[:, :top].astype(jnp.int32)
    weight_all = routing_all[:, top:]
    mine = lax.axis_index("fs") * local_experts + jnp.arange(local_experts, dtype=jnp.int32)
    hit = routes_all[:, None, :, :] == mine[None, :, None, None]
    chosen = jnp.any(hit, axis=2)
    share = jnp.sum(jnp.where(hit, weight_all[:, None, :, :], 0.0), axis=2)
    lower = (jnp.arange(rows)[:, None] <= jnp.arange(rows)[None, :]).astype(jnp.bfloat16)
    count = jnp.einsum(
        "bjt,ts->bjs", chosen.astype(jnp.bfloat16), lower, preferred_element_type=jnp.float32
    )
    slot = jnp.where(chosen, count.astype(jnp.int32) - 1, -1)
    place = slot[:, :, None, :] == jnp.arange(CAP, dtype=jnp.int32)[None, None, :, None]
    pick = place.astype(jnp.bfloat16).reshape(fs_n, local_experts * CAP, rows)
    spread = (
        jnp.where(place, share[:, :, None, :], 0.0)
        .astype(jnp.bfloat16)
        .reshape(fs_n, local_experts * CAP, rows)
    )
    arrived = jnp.einsum(
        "bst,btd->bsd", pick, normed_all, preferred_element_type=jnp.float32
    ).astype(jnp.bfloat16)
    arrived = (
        arrived.reshape(fs_n, local_experts, CAP, width)
        .transpose(1, 0, 2, 3)
        .reshape(local_experts, fs_n * CAP, width)
    )
    def block(array):
        return pl.BlockSpec((None,) + array.shape[1:], lambda e: (e, 0, 0))

    weights = (gate_weight, up_weight, down_weight)
    results, gate_weight, up_weight, down_weight = pl.pallas_call(
        expert_kernel,
        grid=(local_experts,),
        out_shape=[jax.ShapeDtypeStruct(a.shape, jnp.bfloat16) for a in (arrived,) + weights],
        in_specs=[block(a) for a in (arrived,) + weights],
        out_specs=[block(a) for a in (arrived,) + weights],
    )(arrived, *weights)
    results = (
        results.reshape(local_experts, fs_n, CAP, width)
        .transpose(1, 0, 2, 3)
        .reshape(fs_n, local_experts * CAP, width)
    )
    partial_mix = jnp.einsum(
        "bst,bsd->btd", spread, results, preferred_element_type=jnp.float32
    ).astype(jnp.bfloat16)

    in_vmem = pl.BlockSpec(memory_space=pltpu.VMEM)
    half = width // 2
    mixed = pl.pallas_call(
        return_kernel,
        out_shape=jax.ShapeDtypeStruct((rows, half), jnp.bfloat16),
        in_specs=[in_vmem],
        out_specs=in_vmem,
        scratch_shapes=[
            pltpu.VMEM((4, 3, rows, half), jnp.bfloat16),
            pltpu.VMEM((3, rows, half), jnp.bfloat16),
            pltpu.VMEM((3, rows, half), jnp.bfloat16),
            dma((4, 3)), dma((4, 3)), dma((3,)), dma((3,)),
        ],
        compiler_params=pltpu.CompilerParams(collective_id=1, has_side_effects=True),
    )(partial_mix)
    return (mixed, gate_weight, up_weight, down_weight)


def solution(mesh):
    placed = (
        P(("gr", "fs"), None),
        P(("gr", "fs")),
        P(None, ("gr", "fs"), "tp"),
        P(None, ("gr", "fs"), "tp"),
        P(None, ("gr", "fs"), "tp"),
        P(("gr", "fs"), None),
        P(("gr", "fs"), None),
    )
    block = mesh.shape["gr"] == 2 and mesh.shape["fs"] == 8 and mesh.shape["tp"] == 2
    return jax.shard_map(
        body if block else plain_body,
        mesh=mesh,
        in_specs=placed,
        out_specs=(
            P(("gr", "fs"), "tp"),
            P("fs", None, "tp"),
            P("fs", None, "tp"),
            P("fs", "tp", None),
        ),
        check_vma=False,
    )
```
